32 devices in a mesh: ep: 16 (over z, y, x), tp: 2 (over core).
Axes of the slice: x: 2, y: 2, z: 4, core: 2. Of those that a mesh axis runs over, the one named last changes fastest.
Arguments:
- tokens: bfloat16 [16, 2048], P('ep'), may hold values from -6 to 6
- norm_gain: float32 [2048], replicated, may hold values from 0.1 to 1.9
- w_query: bfloat16 [2048, 512], P('ep', 'tp'), may hold values from -0.125 to 0.125
- w_key: bfloat16 [2048, 512], P('ep', 'tp'), may hold values from -0.125 to 0.125
- w_value: bfloat16 [2048, 1024], P('ep', 'tp'), may hold values from -0.125 to 0.125
- w_outgate: bfloat16 [2048, 1024], P('ep', 'tp'), may hold values from -0.125 to 0.125
- decay_in: bfloat16 [2048, 16], replicated, may hold values from -0.125 to 0.125
- decay_out: bfloat16 [16, 512], P(None, 'tp'), may hold values from -1.5 to 1.5
- decay_bias: float32 [512], P('tp'), may hold values from -40 to 4
- gla_state: float32 [16, 2, 256, 512], P('ep', 'tp'), may hold values from -6 to 6
- head_gain: float32 [512], replicated, may hold values from 0.1 to 1.9
- w_output: bfloat16 [1024, 2048], P(None, 'ep'), may hold values from -0.1875 to 0.1875
- moe_gain: float32 [2048], replicated, may hold values from 0.1 to 1.9
- expert_ids: int32 [16, 6], replicated, may hold values from 0 to 15, all different within a row; in each aligned block of 16 rows (0 to 15, 16 to 31, ...) at most 12 rows name the same one
- route_weight: float32 [16, 6], replicated, may hold values from 0.2 to 1
- expert_gate: bfloat16 [16, 2048, 512], P('ep', None, 'tp'), may hold values from -0.125 to 0.125
- expert_up: bfloat16 [16, 2048, 512], P('ep', None, 'tp'), may hold values from -0.125 to 0.125
- expert_down: bfloat16 [16, 512, 2048], P('ep', 'tp'), may hold values from -0.25 to 0.25
- shared_gate: bfloat16 [2048, 512], P(None, 'tp'), may hold values from -0.125 to 0.125
- shared_up: bfloat16 [2048, 512], P(None, 'tp'), may hold values from -0.125 to 0.125
- shared_down: bfloat16 [512, 2048], P('tp'), may hold values from -0.25 to 0.25
Outputs:
- result: bfloat16 [16, 2048], P(None, 'ep')
- new_state: float32 [16, 2, 256, 512], P('ep', 'tp')
The draws below stay inside these ranges and needn't reach their ends.
Inputs may be any that keep to these rules, and one draw needn't show every extreme that they name: `expert_ids`: each row names 6 different experts. No expert is named by more than 12 rows in all, a bound that some block reaches.
All inputs are finite; a program needn't handle non-finite values.
Results may differ from the reference program's by a relative error of at most 0.018.
Values may be sent and summed in bfloat16 or wider, within the bound.
A program may use at most 64 MiB of HBM per device.

```python
import math
import jax
import jax.numpy as jnp
import numpy as np
from jax import lax

D = 2048
HEADS = 2
DK = 256
DV = 512
RANK = 16
F = 512
TOP = 6
TOKENS = 16
EXPERTS = 16
CAP = 12
N_TP = 2


def spiked(values, rng, source, target, parts, factor):
    owner, partner = [(jnp.arange(values.shape[dim]) // (values.shape[dim] // parts)).reshape([-1 if axis == dim else 1 for axis in range(values.ndim)]) for dim in (source, target)]
    chosen = jax.random.permutation(rng, parts)[partner]
    strong = (owner == chosen) | (owner == (partner + parts // 2) % parts)
    return jnp.where(strong, factor * values, values)


def block_levels(own_key, dims, shards, least, high):
    loudness = 1.0
    for dim, shards_of in shards:
        steps = jax.random.uniform(jax.random.fold_in(jax.random.fold_in(own_key, 6), dim), (shards_of,), jnp.float32, least / len(shards), high / len(shards))
        loudness = loudness * jnp.repeat(jnp.exp(steps), dims[dim] // shards_of).reshape((-1,) + (1,) * (len(dims) - 1 - dim))
    return loudness


def deal_out(own_key, own, number, rows, amount, top, most, lean):
    order = jax.random.permutation(own_key, amount)
    packed, usual = load_shares(amount, rows * top, most, lean, True), load_shares(amount, rows * top, most, lean, False)
    places = jnp.arange(amount)

    def named(lengths, turn):
        used = int((lengths > 0).sum())
        fixed = max(1, used // 4)
        passed = fixed + (places - fixed + turn * (used - fixed)) % max(1, amount - fixed)
        return jnp.zeros((amount,), jnp.int32).at[order[jnp.where(places < fixed, places, passed)]].set(jnp.asarray(lengths, jnp.int32))

    lengths = jnp.where(number % 4 == 0, named(packed, number // 4), named(usual, number - number // 4 - 1))
    mixed = jax.random.permutation(jax.random.fold_in(own, 3), amount)
    source_of, taker = mixed[0:amount // 2 * 2:2], mixed[1:amount // 2 * 2:2]
    slack = jnp.minimum(lengths[source_of] - 1, most - lengths[taker]) // 2
    slack = jnp.where((source_of == order[0]) | (taker == order[0]) | (lengths[taker] == 0), 0, jnp.maximum(slack, 0))
    passed = jax.random.randint(jax.random.fold_in(own, 4), (amount // 2,), 0, 1 << 20) % (slack + 1)
    lengths = lengths.at[source_of].add(-passed).at[taker].add(passed)
    items = jnp.searchsorted(jnp.cumsum(lengths), jnp.arange(rows * top), side="right").astype(jnp.int32)
    grid = items.reshape(top, rows).T
    grid = grid[jax.random.permutation(jax.random.fold_in(own, 1), rows)]
    turn = jax.random.randint(jax.random.fold_in(own, 2), (rows, 1), 0, top)
    return jnp.take_along_axis(grid, (jnp.arange(top)[None, :] + turn) % top, axis=1)


def load_shares(count, total, limit, lean, full):
    portions = [(1 << 20) // math.isqrt(standing ** lean) + 1 for standing in range(1, count + 1)]
    largest = limit if full else min(limit, max(-(-total // count), total * portions[0] // sum(portions)))
    least = 1 if total - largest >= count - 1 else 0
    counts, spare = [largest] + [least] * (count - 1), total - largest - least * (count - 1)
    while spare > 0:
        candidates = [i for i in range(1, count) if counts[i] < largest] or [i for i in range(1, count) if counts[i] < limit]
        pool, remaining = sum([portions[i] for i in candidates]), spare
        for i in candidates:
            addition = min(limit - counts[i], max(1, remaining * portions[i] // pool), spare)
            counts[i] = counts[i] + addition
            spare = spare - addition
    return np.array(counts)


def noise(stream_key, dims, scale, reach, cuts=(), kind=jnp.bfloat16):
    array = jax.random.normal(stream_key, dims, jnp.float32) * scale
    if len(cuts) > 0:
        array = block_levels(stream_key, dims, cuts, -0.22, 0.18) * array
    return jnp.clip(array, min=-reach, max=reach).astype(kind)


def heavy_noise(key, extent, scale, limit, shards, heavy, kind=jnp.bfloat16):
    values = scale * jax.random.normal(key, extent, jnp.float32)
    if shards:
        values = values * block_levels(key, extent, shards, -0.22, 0.18)
    return jnp.clip(spiked(values, jax.random.fold_in(key, 3), *heavy), -limit, limit).astype(kind)


def setup_inputs(seed: int = 0) -> dict:
    key_list = jax.random.split(jax.random.key(seed), 22)
    tokens = heavy_noise(key_list[0], (TOKENS, D), 1.0, 6.0, ((0, 16),), (1, 0, 16, 2.0))
    norm_gain = jnp.clip(1.0 + 0.18 * jax.random.normal(key_list[1], (D,), jnp.float32), 0.1, 1.9)
    w_query = noise(key_list[2], (D, HEADS * DK), D ** -0.5, 0.125, ((0, 16), (1, 2)))
    w_key = noise(key_list[3], (D, HEADS * DK), D ** -0.5, 0.125, ((0, 16), (1, 2)))
    w_value = noise(key_list[4], (D, HEADS * DV), D ** -0.5, 0.125, ((0, 16), (1, 2)))
    w_outgate = noise(key_list[5], (D, HEADS * DV), D ** -0.5, 0.125, ((0, 16), (1, 2)))
    decay_in = noise(key_list[6], (D, RANK), D ** -0.5, 0.125)
    decay_out = noise(key_list[7], (RANK, HEADS * DK), RANK ** -0.5, 1.5, ((1, 2),))
    decay_bias = jnp.clip(-40.0 + 44.0 * jax.random.uniform(key_list[8], (HEADS * DK,), jnp.float32) ** block_levels(key_list[8], (HEADS * DK,), ((0, 2),), -0.2, 0.2), -40.0, 4.0)
    gla_state = noise(key_list[9], (TOKENS, HEADS, DK, DV), 1.0, 6.0, ((0, 16), (1, 2)), jnp.float32)
    head_gain = jnp.clip(1.0 + 0.18 * jax.random.normal(key_list[10], (DV,), jnp.float32), 0.1, 1.9)
    w_output = noise(key_list[11], (HEADS * DV, D), (HEADS * DV) ** -0.5, 0.1875, ((1, 16),))
    moe_gain = jnp.clip(1.0 + 0.18 * jax.random.normal(key_list[12], (D,), jnp.float32), 0.1, 1.9)
    expert_ids_keys = jax.random.split(jax.random.fold_in(key_list[13], 1), TOKENS // TOKENS)
    expert_ids_turns = jax.random.permutation(jax.random.fold_in(key_list[13], 3), TOKENS // TOKENS)
    expert_ids = jax.vmap(lambda own, number: deal_out(jax.random.fold_in(key_list[13], 2), own, number, TOKENS, EXPERTS, TOP, CAP, 2))(expert_ids_keys, expert_ids_turns).reshape((TOKENS, TOP))
    route_weight = jnp.clip(jax.random.uniform(key_list[14], (TOKENS, TOP), jnp.float32, 0.2, 1.0), 0.2, 1.0)
    expert_gate = noise(key_list[15], (EXPERTS, D, F), D ** -0.5, 0.125, ((0, 16), (2, 2)))
    expert_up = noise(key_list[16], (EXPERTS, D, F), D ** -0.5, 0.125, ((0, 16), (2, 2)))
    expert_down = noise(key_list[17], (EXPERTS, F, D), F ** -0.5, 0.25, ((0, 16), (1, 2)))
    shared_gate = noise(key_list[18], (D, F), D ** -0.5, 0.125, ((1, 2),))
    shared_up = noise(key_list[19], (D, F), D ** -0.5, 0.125, ((1, 2),))
    shared_down = noise(key_list[20], (F, D), F ** -0.5, 0.25, ((0, 2),))
    return {"tokens": tokens, "norm_gain": norm_gain, "w_query": w_query, "w_key": w_key, "w_value": w_value, "w_outgate": w_outgate, "decay_in": decay_in, "decay_out": decay_out, "decay_bias": decay_bias, "gla_state": gla_state, "head_gain": head_gain, "w_output": w_output, "moe_gain": moe_gain, "expert_ids": expert_ids, "route_weight": route_weight, "expert_gate": expert_gate, "expert_up": expert_up, "expert_down": expert_down, "shared_gate": shared_gate, "shared_up": shared_up, "shared_down": shared_down}


EPSILON = 1e-06
DECAY_TEMPER = 16.0

def rms_scale(values):
    return lax.rsqrt(lax.optimization_barrier(jnp.mean(values * values, axis=-1, keepdims=True)) + EPSILON)

def slot_positions(expert_ids, expert_count):
    flat_ids = expert_ids.reshape(-1).astype(jnp.int32)
    onehot = (flat_ids[:, None] == jnp.arange(expert_count, dtype=jnp.int32)[None, :]).astype(jnp.int32)
    before = jnp.cumsum(onehot, axis=0) - onehot
    position = lax.optimization_barrier(jnp.sum(before * onehot, axis=1)).astype(jnp.int32)
    return (flat_ids, position)

def rounded_add(running, partial_sum):
    held = lax.optimization_barrier(partial_sum.astype(jnp.bfloat16))
    return running + held.astype(jnp.float32)

def swiglu_halves(rows, gate_weight, up_weight, down_weight, halves):
    half_width = gate_weight.shape[1] // halves
    running = jnp.zeros((rows.shape[0], down_weight.shape[1]), jnp.float32)
    for half_index in range(halves):
        lower_edge = half_index * half_width
        upper_edge = lower_edge + half_width
        gate_values = jnp.dot(rows, gate_weight[:, lower_edge:upper_edge], preferred_element_type=jnp.float32)
        upward = jnp.dot(rows, up_weight[:, lower_edge:upper_edge], preferred_element_type=jnp.float32)
        active = (jax.nn.silu(gate_values) * upward).astype(jnp.bfloat16)
        running = rounded_add(running, jnp.dot(active, down_weight[lower_edge:upper_edge], preferred_element_type=jnp.float32))
    return running.astype(jnp.bfloat16)

def reference(tokens, norm_gain, w_query, w_key, w_value, w_outgate, decay_in, decay_out, decay_bias, gla_state, head_gain, w_output, moe_gain, expert_ids, route_weight, expert_gate, expert_up, expert_down, shared_gate, shared_up, shared_down):
    seq_count = tokens.shape[0]
    tok_float = tokens.astype(jnp.float32)
    normed = (tok_float * rms_scale(tok_float) * norm_gain).astype(jnp.bfloat16)
    query_rows = jnp.dot(normed, w_query, preferred_element_type=jnp.float32).astype(jnp.bfloat16)
    key_rows = jnp.dot(normed, w_key, preferred_element_type=jnp.float32).astype(jnp.bfloat16)
    value_rows = jnp.dot(normed, w_value, preferred_element_type=jnp.float32).astype(jnp.bfloat16)
    gate_rows = jnp.dot(normed, w_outgate, preferred_element_type=jnp.float32).astype(jnp.bfloat16)
    decay_low = jnp.dot(normed, decay_in, preferred_element_type=jnp.float32).astype(jnp.bfloat16)
    decay_pre = jnp.dot(decay_low, decay_out, preferred_element_type=jnp.float32) + decay_bias
    decay_rate = jnp.exp(jax.nn.log_sigmoid(decay_pre) / DECAY_TEMPER).reshape(seq_count, HEADS, DK)
    query_heads = query_rows.astype(jnp.float32).reshape(seq_count, HEADS, DK) * DK ** (-0.5)
    key_heads = key_rows.astype(jnp.float32).reshape(seq_count, HEADS, DK)
    value_heads = value_rows.astype(jnp.float32).reshape(seq_count, HEADS, DV)
    new_state = decay_rate[..., None] * gla_state + key_heads[..., None] * value_heads[:, :, None, :]
    read_out = jnp.einsum('shk,shkv->shv', query_heads, new_state, precision=lax.Precision.HIGHEST)
    gate_heads = gate_rows.astype(jnp.float32).reshape(seq_count, HEADS, DV)
    mixed_heads = (read_out * rms_scale(read_out) * head_gain * jax.nn.silu(gate_heads)).astype(jnp.bfloat16)
    mixed_heads = mixed_heads.reshape(seq_count, HEADS * DV)
    attention = jnp.dot(mixed_heads, w_output, preferred_element_type=jnp.float32).astype(jnp.bfloat16)
    hidden = (tok_float + attention.astype(jnp.float32)).astype(jnp.bfloat16)
    hid_float = hidden.astype(jnp.float32)
    hnorm = (hid_float * rms_scale(hid_float) * moe_gain).astype(jnp.bfloat16)
    flat_ids, position = slot_positions(expert_ids, EXPERTS)
    owner_rows = jnp.arange(seq_count * TOP, dtype=jnp.int32) // TOP
    slot_table = jnp.full((EXPERTS, CAP), seq_count, jnp.int32).at[flat_ids, position].set(owner_rows)
    padded = jnp.concatenate([hnorm, jnp.zeros((1, D), jnp.bfloat16)], axis=0)

    def one_expert(operands):
        index_rows, gate_weight, up_weight, down_weight = operands
        return swiglu_halves(padded[index_rows], gate_weight, up_weight, down_weight, N_TP)
    expert_out = lax.map(one_expert, (slot_table, expert_gate, expert_up, expert_down))
    picked = expert_out.reshape(EXPERTS * CAP, D)[(flat_ids * CAP + position).astype(jnp.int32)]
    routed = lax.optimization_barrier(jnp.sum(picked.astype(jnp.float32).reshape(seq_count, TOP, D) * route_weight[..., None], axis=1))
    shared_out = swiglu_halves(hnorm, shared_gate, shared_up, shared_down, N_TP)
    result = (hid_float + routed + shared_out.astype(jnp.float32)).astype(jnp.bfloat16)
    return (result, new_state)
```

```python
import functools

import jax
import jax.numpy as jnp
from jax import lax
from jax.experimental import pallas as pl
from jax.experimental.pallas import tpu as pltpu
from jax.sharding import PartitionSpec as P

DK = 256
DV = 512


EPSILON = 1e-06
DECAY_TEMPER = 16.0


def rms_scale(values):
    return lax.rsqrt(jnp.mean(values * values, axis=-1, keepdims=True) + EPSILON)


def slot_positions(expert_ids, expert_count):
    flat_ids = expert_ids.reshape(-1)
    onehot = (flat_ids[:, None] == jnp.arange(expert_count, dtype=jnp.int32)[None, :]).astype(
        jnp.int32
    )
    before = jnp.cumsum(onehot, axis=0) - onehot
    position = jnp.sum(before * onehot, axis=1)
    return (flat_ids, position)


def expert_block(rows, moe_gain, gate_weight, up_weight, down_weight):
    row_float = rows.astype(jnp.float32)
    normal_rows = (row_float * rms_scale(row_float) * moe_gain).astype(jnp.bfloat16)
    gate_values = jnp.einsum(
        "ecd,edf->ecf", normal_rows, gate_weight, preferred_element_type=jnp.float32
    )
    upward = jnp.einsum("ecd,edf->ecf", normal_rows, up_weight, preferred_element_type=jnp.float32)
    active = (jax.nn.silu(gate_values) * upward).astype(jnp.bfloat16)
    return jnp.einsum(
        "ecf,efd->ecd", active, down_weight, preferred_element_type=jnp.float32
    ).astype(jnp.bfloat16)


def per_device(
    tokens,
    norm_gain,
    w_query,
    w_key,
    w_value,
    w_outgate,
    decay_in,
    decay_out,
    decay_bias,
    gla_state,
    head_gain,
    w_output,
    moe_gain,
    expert_ids,
    route_weight,
    expert_gate,
    expert_up,
    expert_down,
    shared_gate,
    shared_up,
    shared_down,
):
    ep_size = lax.axis_size("ep")
    tp_size = lax.axis_size("tp")
    seq_dev = tokens.shape[0]
    top_count = expert_ids.shape[1]
    exp_dev = expert_gate.shape[0]
    experts = exp_dev * ep_size
    all_rows = seq_dev * ep_size
    capacity = 2 * seq_dev * top_count // exp_dev
    heads_local = w_query.shape[1] // DK
    tok_float = tokens.astype(jnp.float32)
    normed = (tok_float * rms_scale(tok_float) * norm_gain).astype(jnp.bfloat16)
    span_sizes = (w_query.shape[1], w_key.shape[1], w_value.shape[1], w_outgate.shape[1])
    raw_columns, normed_columns = (
        lax.all_to_all(tokens, "ep", split_axis=1, concat_axis=0, tiled=True),
        lax.all_to_all(normed, "ep", split_axis=1, concat_axis=0, tiled=True),
    )
    joined = lax.psum_scatter(
        jnp.concatenate(
            [
                jnp.dot(normed_columns, weight, preferred_element_type=jnp.float32)
                for weight in (w_query, w_key, w_value, w_outgate)
            ],
            axis=1,
        ),
        "ep",
        scatter_dimension=0,
        tiled=True,
    )
    column_edges = [
        0,
        span_sizes[0],
        span_sizes[0] + span_sizes[1],
        span_sizes[0] + span_sizes[1] + span_sizes[2],
        sum(span_sizes),
    ]
    projected = tuple(
        (joined[:, column_edges[number] : column_edges[number + 1]] for number in range(4))
    )
    query_rows, key_rows, value_rows, gate_rows = (
        part_sum.astype(jnp.bfloat16) for part_sum in projected
    )
    decay_low = jnp.dot(normed, decay_in, preferred_element_type=jnp.float32).astype(jnp.bfloat16)
    decay_pre = jnp.dot(decay_low, decay_out, preferred_element_type=jnp.float32) + decay_bias
    decay_rate = jnp.exp(jax.nn.log_sigmoid(decay_pre) / DECAY_TEMPER).reshape(
        seq_dev, heads_local, DK
    )
    query_heads = query_rows.astype(jnp.float32).reshape(seq_dev, heads_local, DK) * DK ** (-0.5)
    key_heads = key_rows.astype(jnp.float32).reshape(seq_dev, heads_local, DK)
    value_heads = value_rows.astype(jnp.float32).reshape(seq_dev, heads_local, DV)
    new_state = (
        decay_rate[..., None] * gla_state + key_heads[..., None] * value_heads[:, :, None, :]
    )
    read_out = jnp.einsum("shk,shkv->shv", query_heads, new_state, precision=lax.Precision.HIGHEST)
    gate_heads = gate_rows.astype(jnp.float32).reshape(seq_dev, heads_local, DV)
    mixed_heads = (read_out * rms_scale(read_out) * head_gain * jax.nn.silu(gate_heads)).astype(
        jnp.bfloat16
    )
    head_weights = w_output.reshape(tp_size, heads_local * DV, w_output.shape[1])
    shard_rows = lax.all_gather(mixed_heads, ("ep", "tp"), axis=0, tiled=True)
    owners = lax.iota(jnp.int32, shard_rows.shape[0])
    select = (owners[:, None] % tp_size == lax.iota(jnp.int32, tp_size)[None, :]).astype(
        jnp.bfloat16
    )
    chosen = jnp.einsum(
        "mt,tcd->mcd", select, head_weights, preferred_element_type=jnp.float32
    ).astype(jnp.bfloat16)
    spread = jnp.einsum("msc,mcd->msd", shard_rows, chosen, preferred_element_type=jnp.float32)
    attention = (
        spread.reshape(ep_size, tp_size, seq_dev, -1)
        .sum(axis=1)
        .reshape(all_rows, -1)
        .astype(jnp.bfloat16)
    )
    hidden = (raw_columns.astype(jnp.float32) + attention.astype(jnp.float32)).astype(jnp.bfloat16)
    flat_ids, position = slot_positions(expert_ids, experts)
    owner_rows = lax.iota(jnp.int32, all_rows * top_count) // top_count
    slot_table = (
        jnp.full((experts, capacity), all_rows, jnp.int32).at[flat_ids, position].set(owner_rows)
    )
    padded = jnp.concatenate([hidden, jnp.zeros((1, hidden.shape[1]), jnp.bfloat16)], axis=0)
    routed_rows, shared_rows = (
        lax.all_to_all(padded[slot_table], "ep", split_axis=0, concat_axis=2, tiled=True),
        lax.all_to_all(
            hidden.reshape(ep_size, seq_dev, hidden.shape[1]),
            "ep",
            split_axis=0,
            concat_axis=2,
            tiled=True,
        ),
    )
    routed_part = expert_block(routed_rows, moe_gain, expert_gate, expert_up, expert_down)
    shared_part = expert_block(
        shared_rows, moe_gain, shared_gate[None], shared_up[None], shared_down[None]
    )
    routed_sum, shared_sum = (
        lax.psum(routed_part, "tp").astype(jnp.float32),
        lax.psum(shared_part, "tp").astype(jnp.float32),
    )
    routed_out = routed_sum.astype(jnp.bfloat16)
    shared_out = shared_sum.astype(jnp.bfloat16)
    back_routed, back_shared = (
        lax.all_to_all(routed_out, "ep", split_axis=2, concat_axis=0, tiled=True),
        lax.all_to_all(shared_out, "ep", split_axis=2, concat_axis=0, tiled=True),
    )
    picked = back_routed.reshape(experts * capacity, -1)[flat_ids * capacity + position]
    weighted = picked.astype(jnp.float32).reshape(all_rows, top_count, -1) * route_weight[..., None]
    moe_columns = jnp.sum(weighted, axis=1) + back_shared.reshape(all_rows, -1).astype(jnp.float32)
    result = (hidden.astype(jnp.float32) + moe_columns).astype(jnp.bfloat16)
    return (result, new_state)


HBM = pltpu.MemorySpace.HBM
MESH = pl.DeviceIdType.MESH


def silu(values):
    return values / (1.0 + jnp.exp(-values))


def rounded(values):
    return values.astype(jnp.bfloat16).astype(jnp.float32)


def layer_kernel(
    ep_size,
    tp_size,
    tokens,
    norm_gain,
    w_query,
    w_key,
    w_value,
    w_outgate,
    decay_in,
    decay_out,
    decay_bias,
    gla_state,
    head_gain,
    w_output,
    moe_gain,
    expert_ids,
    route_weight,
    expert_gate,
    expert_up,
    expert_down,
    shared_gate,
    shared_up,
    shared_down,
    result,
    new_state,
    tok_v,
    gain_v,
    proj_v,
    din_v,
    dout_v,
    bias_v,
    state_v,
    hgain_v,
    wout_v,
    mgain_v,
    ids_v,
    route_v,
    up_v,
    down_v,
    send_a,
    recv_a,
    send_b,
    recv_b,
    send_c,
    recv_c,
    send_d,
    recv_d,
    send_e,
    recv_e,
    result_v,
    local_sem,
    send_sem,
    recv_sem,
):
    me = lax.axis_index("ep")
    core = lax.axis_index("tp")
    devices = ep_size * tp_size
    flat = me * tp_size + core
    block = result_v.shape[1]
    hidden_units = expert_gate.shape[2]
    shared_units = (up_v.shape[1] - 2 * hidden_units) // 2
    shared_blocks = shared_gate.shape[1] // shared_units
    shared_at = pl.multiple_of(lax.rem(me, shared_blocks) * shared_units, shared_units)
    edges = [0]
    for weight in (w_query, w_key, w_value, w_outgate):
        edges.append(edges[-1] + weight.shape[1])

    pending = {}

    def fetch(name, source, target):
        copy = pltpu.make_async_copy(source, target, local_sem.at[len(pending)])
        copy.start()
        pending[name] = copy

    fetch("tokens", tokens, tok_v)
    fetch("norm_gain", norm_gain, gain_v)
    for number, weight in enumerate((w_query, w_key, w_value, w_outgate)):
        fetch(f"proj{number}", weight, proj_v.at[:, pl.ds(edges[number], weight.shape[1])])
    fetch("decay_in", decay_in, din_v)
    fetch("decay_out", decay_out, dout_v)
    fetch("decay_bias", decay_bias, bias_v)
    fetch("state", gla_state.at[0, 0], state_v)
    fetch("head_gain", head_gain, hgain_v)
    fetch("w_output", w_output, wout_v)
    fetch("moe_gain", moe_gain, mgain_v)
    fetch("ids", expert_ids, ids_v)
    fetch("route", route_weight, route_v)
    fetch("gate", expert_gate.at[0], up_v.at[:, pl.ds(0, hidden_units)])
    fetch("up", expert_up.at[0], up_v.at[:, pl.ds(hidden_units, hidden_units)])
    fetch(
        "sgate",
        shared_gate.at[:, pl.ds(shared_at, shared_units)],
        up_v.at[:, pl.ds(2 * hidden_units, shared_units)],
    )
    fetch(
        "sup",
        shared_up.at[:, pl.ds(shared_at, shared_units)],
        up_v.at[:, pl.ds(2 * hidden_units + shared_units, shared_units)],
    )
    fetch("down", expert_down.at[0], down_v.at[pl.ds(0, hidden_units)])
    fetch(
        "sdown",
        shared_down.at[pl.ds(shared_at, shared_units)],
        down_v.at[pl.ds(hidden_units, shared_units)],
    )

    barrier = pltpu.get_barrier_semaphore()

    def to_all(body):
        def step(number, carry):
            other = lax.rem(flat + number, devices)
            body(lax.div(other, tp_size), lax.rem(other, tp_size))
            return carry

        lax.fori_loop(1, devices, step, 0)

    def to_peers(body):
        def step(number, carry):
            body(lax.rem(me + number, ep_size))
            return carry

        lax.fori_loop(1, ep_size, step, 0)

    def remote(source, target, phase, where):
        pltpu.make_async_remote_copy(
            src_ref=source,
            dst_ref=target,
            send_sem=send_sem.at[phase],
            recv_sem=recv_sem.at[phase],
            device_id=where,
            device_id_type=MESH,
        ).start()

    def arrived(span, phase):
        pltpu.make_async_copy(span, span, recv_sem.at[phase]).wait()

    def left(span, phase):
        pltpu.make_async_copy(span, span, send_sem.at[phase]).wait()

    def columns(index):
        return pl.ds(pl.multiple_of(index * block, block), block)

    to_all(lambda e, t: pl.semaphore_signal(barrier, inc=1, device_id=(e, t), device_id_type=MESH))

    pending["tokens"].wait()
    pending["norm_gain"].wait()
    raw = tok_v[...].astype(jnp.float32)
    scale = lax.rsqrt(jnp.mean(raw * raw, axis=-1, keepdims=True) + EPSILON)
    normed = (raw * scale * gain_v[...]).astype(jnp.bfloat16)
    send_a[0:1, :] = normed.astype(jnp.float32)
    send_a[1:2, :] = raw
    recv_a[me] = send_a[:, columns(me)]
    pl.semaphore_wait(barrier, devices - 1)
    to_peers(lambda e: remote(send_a.at[:, columns(e)], recv_a.at[me], 0, (e, core)))

    for name in ("decay_in", "decay_out", "decay_bias", "state"):
        pending[name].wait()
    low = jnp.dot(normed, din_v[...], preferred_element_type=jnp.float32).astype(jnp.bfloat16)
    pre = jnp.dot(low, dout_v[...], preferred_element_type=jnp.float32) + bias_v[...]
    log_sigmoid = jnp.minimum(pre, 0.0) - jnp.log(1.0 + jnp.exp(-jnp.abs(pre)))
    rate = jnp.exp(log_sigmoid / DECAY_TEMPER)
    rate_column = jnp.broadcast_to(rate, (8, DK)).T[:, 0:1]
    state_v[...] = rate_column * state_v[...]

    for number in range(4):
        pending[f"proj{number}"].wait()
    arrived(recv_a.at[pl.ds(0, ep_size - 1)], 0)
    partial = jnp.dot(
        recv_a[:, 0, :].astype(jnp.bfloat16), proj_v[...], preferred_element_type=jnp.float32
    )
    send_b[...] = partial.reshape(send_b.shape)
    recv_b[me] = send_b[me]
    to_peers(lambda e: remote(send_b.at[e], recv_b.at[me], 1, (e, core)))
    for name in ("head_gain", "w_output", "moe_gain", "ids", "route"):
        pending[name].wait()
    arrived(recv_b.at[pl.ds(0, ep_size - 1)], 1)
    joined = rounded(jnp.sum(recv_b[...], axis=0))
    query = joined[:, edges[0] : edges[1]] * DK ** (-0.5)
    key = joined[:, edges[1] : edges[2]]
    value = joined[:, edges[2] : edges[3]]
    gate = joined[:, edges[3] : edges[4]]
    pair = jnp.concatenate(
        [jnp.broadcast_to(key, (4, DK)), jnp.broadcast_to(query, (4, DK))], axis=0
    ).T
    updated = state_v[...] + pair[:, 0:1] * value
    state_v[...] = updated
    read_out = jnp.sum(pair[:, 4:5] * updated, axis=0, keepdims=True)
    read_scale = lax.rsqrt(jnp.mean(read_out * read_out, axis=-1, keepdims=True) + EPSILON)
    mixed = rounded(read_out * read_scale * hgain_v[...] * silu(gate))
    send_c[...] = mixed
    slot = core * ep_size + me
    recv_c[slot] = mixed
    to_all(lambda e, t: remote(send_c, recv_c.at[slot], 2, (e, t)))
    state_out = pltpu.make_async_copy(state_v, new_state.at[0, 0], local_sem.at[len(pending)])
    state_out.start()

    arrived(recv_c.at[pl.ds(0, devices - 1)], 2)
    attention = jnp.zeros((ep_size, block), jnp.float32)
    for head in range(tp_size):
        rows = recv_c[head * ep_size : (head + 1) * ep_size, 0, :].astype(jnp.bfloat16)
        attention = attention + jnp.dot(
            rows, wout_v[head * DV : (head + 1) * DV], preferred_element_type=jnp.float32
        )
    hidden = rounded(recv_a[:, 1, :] + rounded(attention))
    send_d[...] = hidden.astype(jnp.bfloat16)
    recv_d[:, columns(me)] = hidden.astype(jnp.bfloat16)
    to_peers(lambda e: remote(send_d, recv_d.at[:, columns(me)], 3, (e, core)))

    routed = jnp.sum(jnp.where(ids_v[...] == me, route_v[...], 0.0), axis=1, keepdims=True)
    token = lax.broadcasted_iota(jnp.int32, (ep_size, 1), 0)
    shared = jnp.where(
        lax.div(token, shared_blocks) == lax.div(me, shared_blocks), 1.0, 0.0
    )
    for name in ("gate", "up", "sgate", "sup", "down", "sdown"):
        pending[name].wait()
    arrived(recv_d.at[:, pl.ds(0, (ep_size - 1) * block)], 3)
    rows = recv_d[...].astype(jnp.float32)
    row_scale = lax.rsqrt(jnp.mean(rows * rows, axis=-1, keepdims=True) + EPSILON)
    hnorm = (rows * row_scale * mgain_v[...]).astype(jnp.bfloat16)
    both = jnp.dot(hnorm, up_v[...], preferred_element_type=jnp.float32)
    cut = 2 * hidden_units
    active = silu(both[:, :hidden_units]) * both[:, hidden_units:cut] * routed
    extra = silu(both[:, cut : cut + shared_units]) * both[:, cut + shared_units :] * shared
    down = jnp.dot(
        jnp.concatenate([active, extra], axis=1).astype(jnp.bfloat16),
        down_v[...],
        preferred_element_type=jnp.float32,
    )
    send_e[...] = down.astype(jnp.bfloat16)
    recv_e[slot] = send_e[:, columns(me)]
    to_all(lambda e, t: remote(send_e.at[:, columns(e)], recv_e.at[slot], 4, (e, t)))
    arrived(recv_e.at[pl.ds(0, devices - 1)], 4)
    total = jnp.sum(recv_e[...].astype(jnp.float32), axis=0)
    result_v[...] = (hidden + total).astype(jnp.bfloat16)
    result_out = pltpu.make_async_copy(result_v, result, local_sem.at[len(pending) + 1])
    result_out.start()

    left(recv_a.at[pl.ds(0, ep_size - 1)], 0)
    left(recv_b.at[pl.ds(0, ep_size - 1)], 1)
    left(recv_c.at[pl.ds(0, devices - 1)], 2)
    left(recv_d.at[:, pl.ds(0, (ep_size - 1) * block)], 3)
    left(recv_e.at[pl.ds(0, devices - 1)], 4)
    state_out.wait()
    result_out.wait()


def fused_device(*args):
    (
        tokens,
        norm_gain,
        w_query,
        w_key,
        w_value,
        w_outgate,
        decay_in,
        decay_out,
        decay_bias,
        gla_state,
        head_gain,
        w_output,
        moe_gain,
        expert_ids,
        route_weight,
        expert_gate,
        expert_up,
        expert_down,
        shared_gate,
        shared_up,
        shared_down,
    ) = args
    ep_size = lax.axis_size("ep")
    tp_size = lax.axis_size("tp")
    width = tokens.shape[1]
    block = w_output.shape[1]
    span = sum(weight.shape[1] for weight in (w_query, w_key, w_value, w_outgate))
    devices = ep_size * tp_size
    hidden_units = expert_gate.shape[2]
    shared_units = min(128, shared_gate.shape[1])
    rows = [values.reshape(1, -1) for values in (norm_gain, decay_bias, head_gain, moe_gain)]
    operands = (
        tokens,
        rows[0],
        w_query,
        w_key,
        w_value,
        w_outgate,
        decay_in,
        decay_out,
        rows[1],
        gla_state,
        rows[2],
        w_output,
        rows[3],
        expert_ids,
        route_weight,
        expert_gate,
        expert_up,
        expert_down,
        shared_gate,
        shared_up,
        shared_down,
    )

    def held(values):
        return pltpu.VMEM(values.shape, values.dtype)

    scratch = [
        held(tokens),
        held(rows[0]),
        pltpu.VMEM((block, span), jnp.bfloat16),
        held(decay_in),
        held(decay_out),
        held(rows[1]),
        pltpu.VMEM(gla_state.shape[2:], jnp.float32),
        held(rows[2]),
        held(w_output),
        held(rows[3]),
        held(expert_ids),
        held(route_weight),
        pltpu.VMEM((width, 2 * (hidden_units + shared_units)), jnp.bfloat16),
        pltpu.VMEM((hidden_units + shared_units, width), jnp.bfloat16),
        pltpu.VMEM((2, width), jnp.float32),
        pltpu.VMEM((ep_size, 2, block), jnp.float32),
        pltpu.VMEM((ep_size, 1, span), jnp.float32),
        pltpu.VMEM((ep_size, 1, span), jnp.float32),
        pltpu.VMEM((1, DV), jnp.float32),
        pltpu.VMEM((devices, 1, DV), jnp.float32),
        pltpu.VMEM((ep_size, block), jnp.bfloat16),
        pltpu.VMEM((ep_size, width), jnp.bfloat16),
        pltpu.VMEM((ep_size, width), jnp.bfloat16),
        pltpu.VMEM((devices, ep_size, block), jnp.bfloat16),
        pltpu.VMEM((ep_size, block), jnp.bfloat16),
        pltpu.SemaphoreType.DMA((len(operands) + 2,)),
        pltpu.SemaphoreType.DMA((5,)),
        pltpu.SemaphoreType.DMA((5,)),
    ]
    return pl.pallas_call(
        functools.partial(layer_kernel, ep_size, tp_size),
        out_shape=(
            jax.ShapeDtypeStruct((ep_size, block), jnp.bfloat16),
            jax.ShapeDtypeStruct(gla_state.shape, jnp.float32),
        ),
        in_specs=[pl.BlockSpec(memory_space=HBM)] * len(operands),
        out_specs=(pl.BlockSpec(memory_space=HBM), pl.BlockSpec(memory_space=HBM)),
        scratch_shapes=scratch,
        compiler_params=pltpu.CompilerParams(collective_id=0, has_side_effects=True),
    )(*operands)


def chosen_device(*args):
    tokens, w_query, w_output, expert_gate = args[0], args[2], args[11], args[15]
    ep_size = lax.axis_size("ep")
    fits = (
        tokens.shape[0] == 1
        and expert_gate.shape[0] == 1
        and w_query.shape[1] == DK
        and w_output.shape[1] % 128 == 0
        and ep_size % (args[18].shape[1] // min(128, args[18].shape[1])) == 0
    )
    return fused_device(*args) if fits else per_device(*args)


def solution(mesh):
    return jax.shard_map(
        chosen_device,
        mesh=mesh,
        in_specs=(
            P("ep", None),
            P(),
            P("ep", "tp"),
            P("ep", "tp"),
            P("ep", "tp"),
            P("ep", "tp"),
            P(),
            P(None, "tp"),
            P("tp"),
            P("ep", "tp", None, None),
            P(),
            P(None, "ep"),
            P(),
            P(),
            P(),
            P("ep", None, "tp"),
            P("ep", None, "tp"),
            P("ep", "tp", None),
            P(None, "tp"),
            P(None, "tp"),
            P("tp", None),
        ),
        out_specs=(P(None, "ep"), P("ep", "tp", None, None)),
        check_vma=False,
    )
```

```python
import functools

import jax
import jax.numpy as jnp
from jax import lax
from jax.experimental import pallas as pl
from jax.experimental.pallas import tpu as pltpu
from jax.sharding import PartitionSpec as P

DK = 256
DV = 512


EPSILON = 1e-06
DECAY_TEMPER = 16.0


def rms_scale(values):
    return lax.rsqrt(jnp.mean(values * values, axis=-1, keepdims=True) + EPSILON)


def slot_positions(expert_ids, expert_count):
    flat_ids = expert_ids.reshape(-1)
    onehot = (flat_ids[:, None] == jnp.arange(expert_count, dtype=jnp.int32)[None, :]).astype(
        jnp.int32
    )
    before = jnp.cumsum(onehot, axis=0) - onehot
    position = jnp.sum(before * onehot, axis=1)
    return (flat_ids, position)


def expert_block(rows, moe_gain, gate_weight, up_weight, down_weight):
    row_float = rows.astype(jnp.float32)
    normal_rows = (row_float * rms_scale(row_float) * moe_gain).astype(jnp.bfloat16)
    gate_values = jnp.einsum(
        "ecd,edf->ecf", normal_rows, gate_weight, preferred_element_type=jnp.float32
    )
    upward = jnp.einsum("ecd,edf->ecf", normal_rows, up_weight, preferred_element_type=jnp.float32)
    active = (jax.nn.silu(gate_values) * upward).astype(jnp.bfloat16)
    return jnp.einsum(
        "ecf,efd->ecd", active, down_weight, preferred_element_type=jnp.float32
    ).astype(jnp.bfloat16)


def per_device(
    tokens,
    norm_gain,
    w_query,
    w_key,
    w_value,
    w_outgate,
    decay_in,
    decay_out,
    decay_bias,
    gla_state,
    head_gain,
    w_output,
    moe_gain,
    expert_ids,
    route_weight,
    expert_gate,
    expert_up,
    expert_down,
    shared_gate,
    shared_up,
    shared_down,
):
    ep_size = lax.axis_size("ep")
    tp_size = lax.axis_size("tp")
    seq_dev = tokens.shape[0]
    top_count = expert_ids.shape[1]
    exp_dev = expert_gate.shape[0]
    experts = exp_dev * ep_size
    all_rows = seq_dev * ep_size
    capacity = 2 * seq_dev * top_count // exp_dev
    heads_local = w_query.shape[1] // DK
    tok_float = tokens.astype(jnp.float32)
    normed = (tok_float * rms_scale(tok_float) * norm_gain).astype(jnp.bfloat16)
    span_sizes = (w_query.shape[1], w_key.shape[1], w_value.shape[1], w_outgate.shape[1])
    raw_columns, normed_columns = (
        lax.all_to_all(tokens, "ep", split_axis=1, concat_axis=0, tiled=True),
        lax.all_to_all(normed, "ep", split_axis=1, concat_axis=0, tiled=True),
    )
    joined = lax.psum_scatter(
        jnp.concatenate(
            [
                jnp.dot(normed_columns, weight, preferred_element_type=jnp.float32)
                for weight in (w_query, w_key, w_value, w_outgate)
            ],
            axis=1,
        ),
        "ep",
        scatter_dimension=0,
        tiled=True,
    )
    column_edges = [
        0,
        span_sizes[0],
        span_sizes[0] + span_sizes[1],
        span_sizes[0] + span_sizes[1] + span_sizes[2],
        sum(span_sizes),
    ]
    projected = tuple(
        (joined[:, column_edges[number] : column_edges[number + 1]] for number in range(4))
    )
    query_rows, key_rows, value_rows, gate_rows = (
        part_sum.astype(jnp.bfloat16) for part_sum in projected
    )
    decay_low = jnp.dot(normed, decay_in, preferred_element_type=jnp.float32).astype(jnp.bfloat16)
    decay_pre = jnp.dot(decay_low, decay_out, preferred_element_type=jnp.float32) + decay_bias
    decay_rate = jnp.exp(jax.nn.log_sigmoid(decay_pre) / DECAY_TEMPER).reshape(
        seq_dev, heads_local, DK
    )
    query_heads = query_rows.astype(jnp.float32).reshape(seq_dev, heads_local, DK) * DK ** (-0.5)
    key_heads = key_rows.astype(jnp.float32).reshape(seq_dev, heads_local, DK)
    value_heads = value_rows.astype(jnp.float32).reshape(seq_dev, heads_local, DV)
    new_state = (
        decay_rate[..., None] * gla_state + key_heads[..., None] * value_heads[:, :, None, :]
    )
    read_out = jnp.einsum("shk,shkv->shv", query_heads, new_state, precision=lax.Precision.HIGHEST)
    gate_heads = gate_rows.astype(jnp.float32).reshape(seq_dev, heads_local, DV)
    mixed_heads = (read_out * rms_scale(read_out) * head_gain * jax.nn.silu(gate_heads)).astype(
        jnp.bfloat16
    )
    head_weights = w_output.reshape(tp_size, heads_local * DV, w_output.shape[1])
    shard_rows = lax.all_gather(mixed_heads, ("ep", "tp"), axis=0, tiled=True)
    owners = lax.iota(jnp.int32, shard_rows.shape[0])
    select = (owners[:, None] % tp_size == lax.iota(jnp.int32, tp_size)[None, :]).astype(
        jnp.bfloat16
    )
    chosen = jnp.einsum(
        "mt,tcd->mcd", select, head_weights, preferred_element_type=jnp.float32
    ).astype(jnp.bfloat16)
    spread = jnp.einsum("msc,mcd->msd", shard_rows, chosen, preferred_element_type=jnp.float32)
    attention = (
        spread.reshape(ep_size, tp_size, seq_dev, -1)
        .sum(axis=1)
        .reshape(all_rows, -1)
        .astype(jnp.bfloat16)
    )
    hidden = (raw_columns.astype(jnp.float32) + attention.astype(jnp.float32)).astype(jnp.bfloat16)
    flat_ids, position = slot_positions(expert_ids, experts)
    owner_rows = lax.iota(jnp.int32, all_rows * top_count) // top_count
    slot_table = (
        jnp.full((experts, capacity), all_rows, jnp.int32).at[flat_ids, position].set(owner_rows)
    )
    padded = jnp.concatenate([hidden, jnp.zeros((1, hidden.shape[1]), jnp.bfloat16)], axis=0)
    routed_rows, shared_rows = (
        lax.all_to_all(padded[slot_table], "ep", split_axis=0, concat_axis=2, tiled=True),
        lax.all_to_all(
            hidden.reshape(ep_size, seq_dev, hidden.shape[1]),
            "ep",
            split_axis=0,
            concat_axis=2,
            tiled=True,
        ),
    )
    routed_part = expert_block(routed_rows, moe_gain, expert_gate, expert_up, expert_down)
    shared_part = expert_block(
        shared_rows, moe_gain, shared_gate[None], shared_up[None], shared_down[None]
    )
    routed_sum, shared_sum = (
        lax.psum(routed_part, "tp").astype(jnp.float32),
        lax.psum(shared_part, "tp").astype(jnp.float32),
    )
    routed_out = routed_sum.astype(jnp.bfloat16)
    shared_out = shared_sum.astype(jnp.bfloat16)
    back_routed, back_shared = (
        lax.all_to_all(routed_out, "ep", split_axis=2, concat_axis=0, tiled=True),
        lax.all_to_all(shared_out, "ep", split_axis=2, concat_axis=0, tiled=True),
    )
    picked = back_routed.reshape(experts * capacity, -1)[flat_ids * capacity + position]
    weighted = picked.astype(jnp.float32).reshape(all_rows, top_count, -1) * route_weight[..., None]
    moe_columns = jnp.sum(weighted, axis=1) + back_shared.reshape(all_rows, -1).astype(jnp.float32)
    result = (hidden.astype(jnp.float32) + moe_columns).astype(jnp.bfloat16)
    return (result, new_state)


HBM = pltpu.MemorySpace.HBM
MESH = pl.DeviceIdType.MESH


def silu(values):
    return values / (1.0 + jnp.exp(-values))


def rounded(values):
    return values.astype(jnp.bfloat16).astype(jnp.float32)


def layer_kernel(
    ep_size,
    tp_size,
    tokens,
    norm_gain,
    w_query,
    w_key,
    w_value,
    w_outgate,
    decay_in,
    decay_out,
    decay_bias,
    gla_state,
    head_gain,
    w_output,
    moe_gain,
    expert_ids,
    route_weight,
    expert_gate,
    expert_up,
    expert_down,
    shared_gate,
    shared_up,
    shared_down,
    result,
    new_state,
    tok_v,
    gain_v,
    proj_v,
    din_v,
    dout_v,
    bias_v,
    hgain_v,
    wout_v,
    mgain_v,
    ids_v,
    route_v,
    up_v,
    down_v,
    send_a,
    recv_a,
    send_b,
    recv_b,
    send_c,
    recv_c,
    send_d,
    recv_d,
    send_e,
    recv_e,
    local_sem,
    send_sem,
    recv_sem,
):
    me = lax.axis_index("ep")
    core = lax.axis_index("tp")
    devices = ep_size * tp_size
    flat = me * tp_size + core
    block = result.shape[1]
    state_v = new_state.at[0, 0]
    hidden_units = expert_gate.shape[2]
    shared_units = (up_v.shape[1] - 2 * hidden_units) // 2
    shared_blocks = shared_gate.shape[1] // shared_units
    shared_at = pl.multiple_of(lax.rem(me, shared_blocks) * shared_units, shared_units)
    edges = [0]
    for weight in (w_query, w_key, w_value, w_outgate):
        edges.append(edges[-1] + weight.shape[1])

    pending = {}

    def fetch(name, source, target):
        copy = pltpu.make_async_copy(source, target, local_sem.at[len(pending)])
        copy.start()
        pending[name] = copy

    barrier = pltpu.get_barrier_semaphore()

    def wrapped(index, size):
        return jnp.where(index >= size, index - size, index)

    def to_all(body):
        for step in range(ep_size):
            for other in range(tp_size):
                if step or other:
                    body(wrapped(me + step, ep_size), wrapped(core + other, tp_size))

    def to_peers(body):
        for step in range(1, ep_size):
            body(wrapped(me + step, ep_size))

    def remote(source, target, phase, where):
        pltpu.make_async_remote_copy(
            src_ref=source,
            dst_ref=target,
            send_sem=send_sem.at[phase],
            recv_sem=recv_sem.at[phase],
            device_id=where,
            device_id_type=MESH,
        ).start()

    def arrived(span, phase):
        pltpu.make_async_copy(span, span, recv_sem.at[phase]).wait()

    def left(span, phase):
        pltpu.make_async_copy(span, span, send_sem.at[phase]).wait()

    def columns(index):
        return pl.ds(pl.multiple_of(index * block, block), block)

    to_all(lambda e, t: pl.semaphore_signal(barrier, inc=1, device_id=(e, t), device_id_type=MESH))

    fetch("tokens", tokens, tok_v)
    fetch("norm_gain", norm_gain, gain_v)
    for number, weight in enumerate((w_query, w_key, w_value, w_outgate)):
        fetch(f"proj{number}", weight, proj_v.at[:, pl.ds(edges[number], weight.shape[1])])
    fetch("decay_in", decay_in, din_v)
    fetch("decay_out", decay_out, dout_v)
    fetch("decay_bias", decay_bias, bias_v)
    fetch("state", gla_state.at[0, 0], state_v)

    pending["tokens"].wait()
    pending["norm_gain"].wait()
    raw = tok_v[...].astype(jnp.float32)
    scale = lax.rsqrt(jnp.mean(raw * raw, axis=-1, keepdims=True) + EPSILON)
    normed = (raw * scale * gain_v[...]).astype(jnp.bfloat16)
    send_a[0:1, :] = normed.astype(jnp.float32)
    send_a[1:2, :] = raw
    recv_a[me] = send_a[:, columns(me)]
    pl.semaphore_wait(barrier, devices - 1)
    to_peers(lambda e: remote(send_a.at[:, columns(e)], recv_a.at[me], 0, (e, core)))

    fetch("head_gain", head_gain, hgain_v)
    fetch("w_output", w_output, wout_v)
    fetch("moe_gain", moe_gain, mgain_v)
    fetch("ids", expert_ids, ids_v)
    fetch("route", route_weight, route_v)
    fetch("gate", expert_gate.at[0], up_v.at[:, pl.ds(0, hidden_units)])
    fetch("up", expert_up.at[0], up_v.at[:, pl.ds(hidden_units, hidden_units)])
    fetch(
        "sgate",
        shared_gate.at[:, pl.ds(shared_at, shared_units)],
        up_v.at[:, pl.ds(2 * hidden_units, shared_units)],
    )
    fetch(
        "sup",
        shared_up.at[:, pl.ds(shared_at, shared_units)],
        up_v.at[:, pl.ds(2 * hidden_units + shared_units, shared_units)],
    )
    fetch("down", expert_down.at[0], down_v.at[pl.ds(0, hidden_units)])
    fetch(
        "sdown",
        shared_down.at[pl.ds(shared_at, shared_units)],
        down_v.at[pl.ds(hidden_units, shared_units)],
    )

    for name in ("decay_in", "decay_out", "decay_bias", "state"):
        pending[name].wait()
    low = lax.dot_general(
        normed, din_v[...], (((1,), (1,)), ((), ())), preferred_element_type=jnp.float32
    ).astype(jnp.bfloat16)
    pre = jnp.dot(low, dout_v[...], preferred_element_type=jnp.float32) + bias_v[...]
    log_sigmoid = jnp.minimum(pre, 0.0) - jnp.log(1.0 + jnp.exp(-jnp.abs(pre)))
    rate = jnp.exp(log_sigmoid / DECAY_TEMPER)
    rate_column = jnp.broadcast_to(rate, (8, DK)).T[:, 0:1]
    state_v[...] = rate_column * state_v[...]

    for number in range(4):
        pending[f"proj{number}"].wait()
    arrived(recv_a.at[pl.ds(0, ep_size - 1)], 0)
    partial = jnp.dot(
        recv_a[:, 0, :].astype(jnp.bfloat16), proj_v[...], preferred_element_type=jnp.float32
    )
    lanes = send_b.shape[2]
    for number in range(send_b.shape[1]):
        send_b[:, number, :] = partial[:, number * lanes : (number + 1) * lanes].astype(
            jnp.bfloat16
        )
    recv_b[me] = send_b[me]
    to_peers(lambda e: remote(send_b.at[e], recv_b.at[me], 1, (e, core)))
    for name in ("head_gain", "w_output", "moe_gain", "ids", "route"):
        pending[name].wait()
    arrived(recv_b.at[pl.ds(0, ep_size - 1)], 1)
    summed = rounded(jnp.sum(recv_b[...].astype(jnp.float32), axis=0))
    joined = jnp.concatenate(
        [summed[number : number + 1] for number in range(summed.shape[0])], axis=1
    )
    query = joined[:, edges[0] : edges[1]] * DK ** (-0.5)
    key = joined[:, edges[1] : edges[2]]
    value = joined[:, edges[2] : edges[3]]
    gate = joined[:, edges[3] : edges[4]]
    pair = jnp.concatenate(
        [jnp.broadcast_to(key, (4, DK)), jnp.broadcast_to(query, (4, DK))], axis=0
    ).T
    updated = state_v[...] + pair[:, 0:1] * value
    state_v[...] = updated
    read_out = jnp.sum(pair[:, 4:5] * updated, axis=0, keepdims=True)
    read_scale = lax.rsqrt(jnp.mean(read_out * read_out, axis=-1, keepdims=True) + EPSILON)
    mixed = rounded(read_out * read_scale * hgain_v[...] * silu(gate))
    packed = jnp.concatenate(
        [mixed[:, part * lanes : (part + 1) * lanes] for part in range(send_c.shape[0])], axis=0
    ).astype(jnp.bfloat16)
    send_c[...] = packed
    slot = core * ep_size + me
    recv_c[slot] = packed
    to_all(lambda e, t: remote(send_c, recv_c.at[slot], 2, (e, t)))

    arrived(recv_c.at[pl.ds(0, devices - 1)], 2)
    attention = jnp.zeros((ep_size, block), jnp.float32)
    for head in range(tp_size):
        heads = recv_c[head * ep_size : (head + 1) * ep_size].astype(jnp.float32)
        rows = jnp.concatenate(
            [heads[:, part, :] for part in range(send_c.shape[0])], axis=1
        ).astype(jnp.bfloat16)
        attention = attention + jnp.dot(
            rows, wout_v[head * DV : (head + 1) * DV], preferred_element_type=jnp.float32
        )
    hidden = rounded(recv_a[:, 1, :] + rounded(attention))
    send_d[...] = hidden.astype(jnp.bfloat16)
    recv_d[:, columns(me)] = hidden.astype(jnp.bfloat16)
    to_peers(lambda e: remote(send_d, recv_d.at[:, columns(me)], 3, (e, core)))

    chosen = jnp.sum(jnp.where(ids_v[...] == me, route_v[...], 0.0), axis=0, keepdims=True)
    square = (ep_size, ep_size)
    diagonal = lax.broadcasted_iota(jnp.int32, square, 0) == lax.broadcasted_iota(
        jnp.int32, square, 1
    )
    routed = jnp.sum(jnp.where(diagonal, chosen, 0.0), axis=1, keepdims=True)
    token = lax.broadcasted_iota(jnp.int32, (ep_size, 1), 0)
    shared = jnp.where(
        lax.div(token, shared_blocks) == lax.div(me, shared_blocks), 1.0, 0.0
    )
    for name in ("gate", "up", "sgate", "sup", "down", "sdown"):
        pending[name].wait()
    arrived(recv_d.at[:, pl.ds(0, (ep_size - 1) * block)], 3)
    rows = recv_d[...].astype(jnp.float32)
    row_scale = lax.rsqrt(jnp.mean(rows * rows, axis=-1, keepdims=True) + EPSILON)
    hnorm = (rows * row_scale * mgain_v[...]).astype(jnp.bfloat16)
    both = jnp.dot(hnorm, up_v[...], preferred_element_type=jnp.float32)
    cut = 2 * hidden_units
    active = silu(both[:, :hidden_units]) * both[:, hidden_units:cut] * routed
    extra = silu(both[:, cut : cut + shared_units]) * both[:, cut + shared_units :] * shared
    down = jnp.dot(
        jnp.concatenate([active, extra], axis=1).astype(jnp.bfloat16),
        down_v[...],
        preferred_element_type=jnp.float32,
    )
    send_e[...] = down.astype(jnp.bfloat16)
    recv_e[slot] = send_e[:, columns(me)]
    to_all(lambda e, t: remote(send_e.at[:, columns(e)], recv_e.at[slot], 4, (e, t)))
    arrived(recv_e.at[pl.ds(0, devices - 1)], 4)
    total = jnp.sum(recv_e[...].astype(jnp.float32), axis=0)
    result[...] = (hidden + total).astype(jnp.bfloat16)

    left(recv_a.at[pl.ds(0, ep_size - 1)], 0)
    left(recv_b.at[pl.ds(0, ep_size - 1)], 1)
    left(recv_c.at[pl.ds(0, devices - 1)], 2)
    left(recv_d.at[:, pl.ds(0, (ep_size - 1) * block)], 3)
    left(recv_e.at[pl.ds(0, devices - 1)], 4)


def write_kernel(result, state, result_out, state_out, sems):
    copies = [
        pltpu.make_async_copy(state, state_out, sems.at[0]),
        pltpu.make_async_copy(result, result_out, sems.at[1]),
    ]
    for copy in copies:
        copy.start()
    for copy in copies:
        copy.wait()


def fused_device(*args):
    (
        tokens,
        norm_gain,
        w_query,
        w_key,
        w_value,
        w_outgate,
        decay_in,
        decay_out,
        decay_bias,
        gla_state,
        head_gain,
        w_output,
        moe_gain,
        expert_ids,
        route_weight,
        expert_gate,
        expert_up,
        expert_down,
        shared_gate,
        shared_up,
        shared_down,
    ) = args
    ep_size = lax.axis_size("ep")
    tp_size = lax.axis_size("tp")
    width = tokens.shape[1]
    block = w_output.shape[1]
    span = sum(weight.shape[1] for weight in (w_query, w_key, w_value, w_outgate))
    devices = ep_size * tp_size
    hidden_units = expert_gate.shape[2]
    shared_units = min(128, shared_gate.shape[1])
    rows = [values.reshape(1, -1) for values in (norm_gain, decay_bias, head_gain, moe_gain)]
    operands = (
        tokens,
        rows[0],
        w_query,
        w_key,
        w_value,
        w_outgate,
        decay_in.T,
        decay_out,
        rows[1],
        gla_state,
        rows[2],
        w_output,
        rows[3],
        expert_ids.T,
        route_weight.T,
        expert_gate,
        expert_up,
        expert_down,
        shared_gate,
        shared_up,
        shared_down,
    )

    def held(values):
        return pltpu.VMEM(values.shape, values.dtype)

    scratch = [
        held(tokens),
        held(rows[0]),
        pltpu.VMEM((block, span), jnp.bfloat16),
        held(operands[6]),
        held(decay_out),
        held(rows[1]),
        held(rows[2]),
        held(w_output),
        held(rows[3]),
        held(operands[13]),
        held(operands[14]),
        pltpu.VMEM((width, 2 * (hidden_units + shared_units)), jnp.bfloat16),
        pltpu.VMEM((hidden_units + shared_units, width), jnp.bfloat16),
        pltpu.VMEM((2, width), jnp.float32),
        pltpu.VMEM((ep_size, 2, block), jnp.float32),
        pltpu.VMEM((ep_size, span // 128, 128), jnp.bfloat16),
        pltpu.VMEM((ep_size, span // 128, 128), jnp.bfloat16),
        pltpu.VMEM((DV // 128, 128), jnp.bfloat16),
        pltpu.VMEM((devices, DV // 128, 128), jnp.bfloat16),
        pltpu.VMEM((ep_size, block), jnp.bfloat16),
        pltpu.VMEM((ep_size, width), jnp.bfloat16),
        pltpu.VMEM((ep_size, width), jnp.bfloat16),
        pltpu.VMEM((devices, ep_size, block), jnp.bfloat16),
        pltpu.SemaphoreType.DMA((len(operands),)),
        pltpu.SemaphoreType.DMA((5,)),
        pltpu.SemaphoreType.DMA((5,)),
    ]
    result, new_state = pl.pallas_call(
        functools.partial(layer_kernel, ep_size, tp_size),
        out_shape=(
            pltpu.VMEM((ep_size, block), jnp.bfloat16),
            pltpu.VMEM(gla_state.shape, jnp.float32),
        ),
        in_specs=[pl.BlockSpec(memory_space=HBM)] * len(operands),
        out_specs=(pl.BlockSpec(memory_space=pltpu.VMEM),) * 2,
        scratch_shapes=scratch,
        compiler_params=pltpu.CompilerParams(
            collective_id=0, has_side_effects=True
        ),
    )(*operands)
    return pl.pallas_call(
        write_kernel,
        out_shape=(
            jax.ShapeDtypeStruct(result.shape, result.dtype),
            jax.ShapeDtypeStruct(new_state.shape, new_state.dtype),
        ),
        in_specs=[pl.BlockSpec(memory_space=pltpu.VMEM)] * 2,
        out_specs=(pl.BlockSpec(memory_space=HBM),) * 2,
        scratch_shapes=[pltpu.SemaphoreType.DMA((2,))],
        compiler_params=pltpu.CompilerParams(vmem_limit_bytes=8 * 1024 * 1024),
    )(result, new_state)


def chosen_device(*args):
    tokens, w_query, w_output, expert_gate = args[0], args[2], args[11], args[15]
    ep_size = lax.axis_size("ep")
    fits = (
        tokens.shape[0] == 1
        and expert_gate.shape[0] == 1
        and w_query.shape[1] == DK
        and w_output.shape[1] % 128 == 0
        and ep_size % (args[18].shape[1] // min(128, args[18].shape[1])) == 0
    )
    return fused_device(*args) if fits else per_device(*args)


def solution(mesh):
    return jax.shard_map(
        chosen_device,
        mesh=mesh,
        in_specs=(
            P("ep", None),
            P(),
            P("ep", "tp"),
            P("ep", "tp"),
            P("ep", "tp"),
            P("ep", "tp"),
            P(),
            P(None, "tp"),
            P("tp"),
            P("ep", "tp", None, None),
            P(),
            P(None, "ep"),
            P(),
            P(),
            P(),
            P("ep", None, "tp"),
            P("ep", None, "tp"),
            P("ep", "tp", None),
            P(None, "tp"),
            P(None, "tp"),
            P("tp", None),
        ),
        out_specs=(P(None, "ep"), P("ep", "tp", None, None)),
        check_vma=False,
    )
```

```python
import functools

import jax
import jax.numpy as jnp
from jax import lax
from jax.experimental import pallas as pl
from jax.experimental.pallas import tpu as pltpu
from jax.sharding import PartitionSpec as P

DK = 256
DV = 512


EPSILON = 1e-06
DECAY_TEMPER = 16.0


def rms_scale(values):
    return lax.rsqrt(jnp.mean(values * values, axis=-1, keepdims=True) + EPSILON)


def slot_positions(expert_ids, expert_count):
    flat_ids = expert_ids.reshape(-1)
    onehot = (flat_ids[:, None] == jnp.arange(expert_count, dtype=jnp.int32)[None, :]).astype(
        jnp.int32
    )
    before = jnp.cumsum(onehot, axis=0) - onehot
    position = jnp.sum(before * onehot, axis=1)
    return (flat_ids, position)


def expert_block(rows, moe_gain, gate_weight, up_weight, down_weight):
    row_float = rows.astype(jnp.float32)
    normal_rows = (row_float * rms_scale(row_float) * moe_gain).astype(jnp.bfloat16)
    gate_values = jnp.einsum(
        "ecd,edf->ecf", normal_rows, gate_weight, preferred_element_type=jnp.float32
    )
    upward = jnp.einsum("ecd,edf->ecf", normal_rows, up_weight, preferred_element_type=jnp.float32)
    active = (jax.nn.silu(gate_values) * upward).astype(jnp.bfloat16)
    return jnp.einsum(
        "ecf,efd->ecd", active, down_weight, preferred_element_type=jnp.float32
    ).astype(jnp.bfloat16)


def per_device(
    tokens,
    norm_gain,
    w_query,
    w_key,
    w_value,
    w_outgate,
    decay_in,
    decay_out,
    decay_bias,
    gla_state,
    head_gain,
    w_output,
    moe_gain,
    expert_ids,
    route_weight,
    expert_gate,
    expert_up,
    expert_down,
    shared_gate,
    shared_up,
    shared_down,
):
    ep_size = lax.axis_size("ep")
    tp_size = lax.axis_size("tp")
    seq_dev = tokens.shape[0]
    top_count = expert_ids.shape[1]
    exp_dev = expert_gate.shape[0]
    experts = exp_dev * ep_size
    all_rows = seq_dev * ep_size
    capacity = 2 * seq_dev * top_count // exp_dev
    heads_local = w_query.shape[1] // DK
    tok_float = tokens.astype(jnp.float32)
    normed = (tok_float * rms_scale(tok_float) * norm_gain).astype(jnp.bfloat16)
    span_sizes = (w_query.shape[1], w_key.shape[1], w_value.shape[1], w_outgate.shape[1])
    raw_columns, normed_columns = (
        lax.all_to_all(tokens, "ep", split_axis=1, concat_axis=0, tiled=True),
        lax.all_to_all(normed, "ep", split_axis=1, concat_axis=0, tiled=True),
    )
    joined = lax.psum_scatter(
        jnp.concatenate(
            [
                jnp.dot(normed_columns, weight, preferred_element_type=jnp.float32)
                for weight in (w_query, w_key, w_value, w_outgate)
            ],
            axis=1,
        ),
        "ep",
        scatter_dimension=0,
        tiled=True,
    )
    column_edges = [
        0,
        span_sizes[0],
        span_sizes[0] + span_sizes[1],
        span_sizes[0] + span_sizes[1] + span_sizes[2],
        sum(span_sizes),
    ]
    projected = tuple(
        (joined[:, column_edges[number] : column_edges[number + 1]] for number in range(4))
    )
    query_rows, key_rows, value_rows, gate_rows = (
        part_sum.astype(jnp.bfloat16) for part_sum in projected
    )
    decay_low = jnp.dot(normed, decay_in, preferred_element_type=jnp.float32).astype(jnp.bfloat16)
    decay_pre = jnp.dot(decay_low, decay_out, preferred_element_type=jnp.float32) + decay_bias
    decay_rate = jnp.exp(jax.nn.log_sigmoid(decay_pre) / DECAY_TEMPER).reshape(
        seq_dev, heads_local, DK
    )
    query_heads = query_rows.astype(jnp.float32).reshape(seq_dev, heads_local, DK) * DK ** (-0.5)
    key_heads = key_rows.astype(jnp.float32).reshape(seq_dev, heads_local, DK)
    value_heads = value_rows.astype(jnp.float32).reshape(seq_dev, heads_local, DV)
    new_state = (
        decay_rate[..., None] * gla_state + key_heads[..., None] * value_heads[:, :, None, :]
    )
    read_out = jnp.einsum("shk,shkv->shv", query_heads, new_state, precision=lax.Precision.HIGHEST)
    gate_heads = gate_rows.astype(jnp.float32).reshape(seq_dev, heads_local, DV)
    mixed_heads = (read_out * rms_scale(read_out) * head_gain * jax.nn.silu(gate_heads)).astype(
        jnp.bfloat16
    )
    head_weights = w_output.reshape(tp_size, heads_local * DV, w_output.shape[1])
    shard_rows = lax.all_gather(mixed_heads, ("ep", "tp"), axis=0, tiled=True)
    owners = lax.iota(jnp.int32, shard_rows.shape[0])
    select = (owners[:, None] % tp_size == lax.iota(jnp.int32, tp_size)[None, :]).astype(
        jnp.bfloat16
    )
    chosen = jnp.einsum(
        "mt,tcd->mcd", select, head_weights, preferred_element_type=jnp.float32
    ).astype(jnp.bfloat16)
    spread = jnp.einsum("msc,mcd->msd", shard_rows, chosen, preferred_element_type=jnp.float32)
    attention = (
        spread.reshape(ep_size, tp_size, seq_dev, -1)
        .sum(axis=1)
        .reshape(all_rows, -1)
        .astype(jnp.bfloat16)
    )
    hidden = (raw_columns.astype(jnp.float32) + attention.astype(jnp.float32)).astype(jnp.bfloat16)
    flat_ids, position = slot_positions(expert_ids, experts)
    owner_rows = lax.iota(jnp.int32, all_rows * top_count) // top_count
    slot_table = (
        jnp.full((experts, capacity), all_rows, jnp.int32).at[flat_ids, position].set(owner_rows)
    )
    padded = jnp.concatenate([hidden, jnp.zeros((1, hidden.shape[1]), jnp.bfloat16)], axis=0)
    routed_rows, shared_rows = (
        lax.all_to_all(padded[slot_table], "ep", split_axis=0, concat_axis=2, tiled=True),
        lax.all_to_all(
            hidden.reshape(ep_size, seq_dev, hidden.shape[1]),
            "ep",
            split_axis=0,
            concat_axis=2,
            tiled=True,
        ),
    )
    routed_part = expert_block(routed_rows, moe_gain, expert_gate, expert_up, expert_down)
    shared_part = expert_block(
        shared_rows, moe_gain, shared_gate[None], shared_up[None], shared_down[None]
    )
    routed_sum, shared_sum = (
        lax.psum(routed_part, "tp").astype(jnp.float32),
        lax.psum(shared_part, "tp").astype(jnp.float32),
    )
    routed_out = routed_sum.astype(jnp.bfloat16)
    shared_out = shared_sum.astype(jnp.bfloat16)
    back_routed, back_shared = (
        lax.all_to_all(routed_out, "ep", split_axis=2, concat_axis=0, tiled=True),
        lax.all_to_all(shared_out, "ep", split_axis=2, concat_axis=0, tiled=True),
    )
    picked = back_routed.reshape(experts * capacity, -1)[flat_ids * capacity + position]
    weighted = picked.astype(jnp.float32).reshape(all_rows, top_count, -1) * route_weight[..., None]
    moe_columns = jnp.sum(weighted, axis=1) + back_shared.reshape(all_rows, -1).astype(jnp.float32)
    result = (hidden.astype(jnp.float32) + moe_columns).astype(jnp.bfloat16)
    return (result, new_state)


HBM = pltpu.MemorySpace.HBM
MESH = pl.DeviceIdType.MESH


def silu(values):
    return values / (1.0 + jnp.exp(-values))


def rounded(values):
    return values.astype(jnp.bfloat16).astype(jnp.float32)


def layer_kernel(
    ep_size,
    tp_size,
    tokens,
    norm_gain,
    w_query,
    w_key,
    w_value,
    w_outgate,
    decay_in,
    decay_out,
    decay_bias,
    gla_state,
    head_gain,
    w_output,
    moe_gain,
    expert_ids,
    route_weight,
    expert_gate,
    expert_up,
    expert_down,
    shared_gate,
    shared_up,
    shared_down,
    result,
    new_state,
    tok_v,
    gain_v,
    proj_v,
    din_v,
    dout_v,
    bias_v,
    hgain_v,
    wout_v,
    mgain_v,
    ids_v,
    route_v,
    up_v,
    down_v,
    send_a,
    recv_a,
    send_b,
    recv_b,
    send_c,
    recv_c,
    send_d,
    recv_d,
    send_e,
    recv_e,
    stage,
    local_sem,
    send_sem,
    recv_sem,
):
    me = lax.axis_index("ep")
    core = lax.axis_index("tp")
    devices = ep_size * tp_size
    flat = me * tp_size + core
    block = result.shape[1]
    state_v = new_state.at[0, 0]
    hidden_units = expert_gate.shape[2]
    shared_units = (up_v.shape[1] - 2 * hidden_units) // 2
    shared_blocks = shared_gate.shape[1] // shared_units
    shared_at = pl.multiple_of(lax.rem(me, shared_blocks) * shared_units, shared_units)
    edges = [0]
    for weight in (w_query, w_key, w_value, w_outgate):
        edges.append(edges[-1] + weight.shape[1])

    pending = {}

    def fetch(name, source, target):
        copy = pltpu.make_async_copy(source, target, local_sem.at[len(pending)])
        copy.start()
        pending[name] = copy

    barrier = pltpu.get_barrier_semaphore()

    def wrapped(index, size):
        return jnp.where(index >= size, index - size, index)

    def to_all(body):
        for step in range(ep_size):
            for other in range(tp_size):
                if step or other:
                    body(wrapped(me + step, ep_size), wrapped(core + other, tp_size))

    def to_peers(body):
        for step in range(1, ep_size):
            body(wrapped(me + step, ep_size))

    def remote(source, target, phase, where):
        pltpu.make_async_remote_copy(
            src_ref=source,
            dst_ref=target,
            send_sem=send_sem.at[phase],
            recv_sem=recv_sem.at[phase],
            device_id=where,
            device_id_type=MESH,
        ).start()

    def arrived(span, phase):
        pltpu.make_async_copy(span, span, recv_sem.at[phase]).wait()

    def left(span, phase):
        pltpu.make_async_copy(span, span, send_sem.at[phase]).wait()

    def columns(index):
        return pl.ds(pl.multiple_of(index * block, block), block)

    to_all(lambda e, t: pl.semaphore_signal(barrier, inc=1, device_id=(e, t), device_id_type=MESH))

    fetch("tokens", tokens, tok_v)
    fetch("norm_gain", norm_gain, gain_v)
    for number, weight in enumerate((w_query, w_key, w_value, w_outgate)):
        fetch(f"proj{number}", weight, proj_v.at[:, pl.ds(edges[number], weight.shape[1])])
    fetch("decay_in", decay_in, din_v)
    fetch("decay_out", decay_out, dout_v)
    fetch("decay_bias", decay_bias, bias_v)
    fetch("state", gla_state.at[0, 0], state_v)

    pending["tokens"].wait()
    pending["norm_gain"].wait()
    raw = tok_v[...].astype(jnp.float32)
    scale = lax.rsqrt(jnp.mean(raw * raw, axis=-1, keepdims=True) + EPSILON)
    normed = (raw * scale * gain_v[...]).astype(jnp.bfloat16)
    send_a[0:1, :] = normed.astype(jnp.float32)
    send_a[1:2, :] = raw
    recv_a[me] = send_a[:, columns(me)]
    pl.semaphore_wait(barrier, devices - 1)
    to_peers(lambda e: remote(send_a.at[:, columns(e)], recv_a.at[me], 0, (e, core)))

    fetch("head_gain", head_gain, hgain_v)
    fetch("w_output", w_output, wout_v)
    fetch("moe_gain", moe_gain, mgain_v)
    fetch("ids", expert_ids, ids_v)
    fetch("route", route_weight, route_v)
    fetch("gate", expert_gate.at[0], up_v.at[:, pl.ds(0, hidden_units)])
    fetch("up", expert_up.at[0], up_v.at[:, pl.ds(hidden_units, hidden_units)])
    fetch(
        "sgate",
        shared_gate.at[:, pl.ds(shared_at, shared_units)],
        up_v.at[:, pl.ds(2 * hidden_units, shared_units)],
    )
    fetch(
        "sup",
        shared_up.at[:, pl.ds(shared_at, shared_units)],
        up_v.at[:, pl.ds(2 * hidden_units + shared_units, shared_units)],
    )
    fetch("down", expert_down.at[0], down_v.at[pl.ds(0, hidden_units)])
    fetch(
        "sdown",
        shared_down.at[pl.ds(shared_at, shared_units)],
        down_v.at[pl.ds(hidden_units, shared_units)],
    )

    for name in ("decay_in", "decay_out", "decay_bias", "state"):
        pending[name].wait()
    low = lax.dot_general(
        normed, din_v[...], (((1,), (1,)), ((), ())), preferred_element_type=jnp.float32
    ).astype(jnp.bfloat16)
    pre = jnp.dot(low, dout_v[...], preferred_element_type=jnp.float32) + bias_v[...]
    log_sigmoid = jnp.minimum(pre, 0.0) - jnp.log(1.0 + jnp.exp(-jnp.abs(pre)))
    rate = jnp.exp(log_sigmoid / DECAY_TEMPER)
    rate_column = jnp.broadcast_to(rate, (8, DK)).T[:, 0:1]
    state_v[...] = rate_column * state_v[...]

    for number in range(4):
        pending[f"proj{number}"].wait()
    arrived(recv_a.at[pl.ds(0, ep_size - 1)], 0)
    partial = jnp.dot(
        recv_a[:, 0, :].astype(jnp.bfloat16), proj_v[...], preferred_element_type=jnp.float32
    )
    lanes = send_b.shape[2]
    for number in range(send_b.shape[1]):
        stage[:, number, :] = partial[:, number * lanes : (number + 1) * lanes]
    send_b[...] = stage[...].astype(jnp.bfloat16)
    recv_b[me] = send_b[me]
    to_peers(lambda e: remote(send_b.at[e], recv_b.at[me], 1, (e, core)))
    for name in ("head_gain", "w_output", "moe_gain", "ids", "route"):
        pending[name].wait()
    arrived(recv_b.at[pl.ds(0, ep_size - 1)], 1)
    summed = rounded(jnp.sum(recv_b[...].astype(jnp.float32), axis=0))
    joined = jnp.concatenate(
        [summed[number : number + 1] for number in range(summed.shape[0])], axis=1
    )
    query = joined[:, edges[0] : edges[1]] * DK ** (-0.5)
    key = joined[:, edges[1] : edges[2]]
    value = joined[:, edges[2] : edges[3]]
    gate = joined[:, edges[3] : edges[4]]
    pair = jnp.concatenate(
        [jnp.broadcast_to(key, (4, DK)), jnp.broadcast_to(query, (4, DK))], axis=0
    ).T
    read_out = (
        jnp.sum(pair[:, 4:5] * state_v[...], axis=0, keepdims=True)
        + jnp.sum(query * key, axis=-1, keepdims=True) * value
    )
    read_scale = lax.rsqrt(jnp.mean(read_out * read_out, axis=-1, keepdims=True) + EPSILON)
    mixed = rounded(read_out * read_scale * hgain_v[...] * silu(gate))
    packed = jnp.concatenate(
        [mixed[:, part * lanes : (part + 1) * lanes] for part in range(send_c.shape[0])], axis=0
    ).astype(jnp.bfloat16)
    send_c[...] = packed
    slot = core * ep_size + me
    recv_c[slot] = packed
    to_all(lambda e, t: remote(send_c, recv_c.at[slot], 2, (e, t)))
    state_v[...] = state_v[...] + pair[:, 0:1] * value

    arrived(recv_c.at[pl.ds(0, devices - 1)], 2)
    attention = jnp.zeros((ep_size, block), jnp.float32)
    for head in range(tp_size):
        heads = recv_c[head * ep_size : (head + 1) * ep_size].astype(jnp.float32)
        rows = jnp.concatenate(
            [heads[:, part, :] for part in range(send_c.shape[0])], axis=1
        ).astype(jnp.bfloat16)
        attention = attention + jnp.dot(
            rows, wout_v[head * DV : (head + 1) * DV], preferred_element_type=jnp.float32
        )
    hidden = rounded(recv_a[:, 1, :] + rounded(attention))
    send_d[...] = hidden.astype(jnp.bfloat16)
    recv_d[:, columns(me)] = hidden.astype(jnp.bfloat16)
    to_peers(lambda e: remote(send_d, recv_d.at[:, columns(me)], 3, (e, core)))

    chosen = jnp.sum(jnp.where(ids_v[...] == me, route_v[...], 0.0), axis=0, keepdims=True)
    square = (ep_size, ep_size)
    diagonal = lax.broadcasted_iota(jnp.int32, square, 0) == lax.broadcasted_iota(
        jnp.int32, square, 1
    )
    routed = jnp.sum(jnp.where(diagonal, chosen, 0.0), axis=1, keepdims=True)
    token = lax.broadcasted_iota(jnp.int32, (ep_size, 1), 0)
    shared = jnp.where(
        lax.div(token, shared_blocks) == lax.div(me, shared_blocks), 1.0, 0.0
    )
    for name in ("gate", "up", "sgate", "sup", "down", "sdown"):
        pending[name].wait()
    arrived(recv_d.at[:, pl.ds(0, (ep_size - 1) * block)], 3)
    rows = recv_d[...].astype(jnp.float32)
    row_scale = lax.rsqrt(jnp.mean(rows * rows, axis=-1, keepdims=True) + EPSILON)
    gained = (rows * mgain_v[...]).astype(jnp.bfloat16)
    both = jnp.dot(gained, up_v[...], preferred_element_type=jnp.float32) * row_scale
    cut = 2 * hidden_units
    active = silu(both[:, :hidden_units]) * both[:, hidden_units:cut] * routed
    extra = silu(both[:, cut : cut + shared_units]) * both[:, cut + shared_units :] * shared
    down = jnp.dot(
        jnp.concatenate([active, extra], axis=1).astype(jnp.bfloat16),
        down_v[...],
        preferred_element_type=jnp.float32,
    )
    send_e[...] = down.astype(jnp.bfloat16)
    recv_e[slot] = send_e[:, columns(me)]
    to_all(lambda e, t: remote(send_e.at[:, columns(e)], recv_e.at[slot], 4, (e, t)))
    arrived(recv_e.at[pl.ds(0, devices - 1)], 4)
    total = jnp.sum(recv_e[...].astype(jnp.float32), axis=0)
    result[...] = (hidden + total).astype(jnp.bfloat16)

    left(recv_a.at[pl.ds(0, ep_size - 1)], 0)
    left(recv_b.at[pl.ds(0, ep_size - 1)], 1)
    left(recv_c.at[pl.ds(0, devices - 1)], 2)
    left(recv_d.at[:, pl.ds(0, (ep_size - 1) * block)], 3)
    left(recv_e.at[pl.ds(0, devices - 1)], 4)


def write_kernel(result, state, result_out, state_out, sems):
    copies = [
        pltpu.make_async_copy(state, state_out, sems.at[0]),
        pltpu.make_async_copy(result, result_out, sems.at[1]),
    ]
    for copy in copies:
        copy.start()
    for copy in copies:
        copy.wait()


def fused_device(*args):
    (
        tokens,
        norm_gain,
        w_query,
        w_key,
        w_value,
        w_outgate,
        decay_in,
        decay_out,
        decay_bias,
        gla_state,
        head_gain,
        w_output,
        moe_gain,
        expert_ids,
        route_weight,
        expert_gate,
        expert_up,
        expert_down,
        shared_gate,
        shared_up,
        shared_down,
    ) = args
    ep_size = lax.axis_size("ep")
    tp_size = lax.axis_size("tp")
    width = tokens.shape[1]
    block = w_output.shape[1]
    span = sum(weight.shape[1] for weight in (w_query, w_key, w_value, w_outgate))
    devices = ep_size * tp_size
    hidden_units = expert_gate.shape[2]
    shared_units = min(128, shared_gate.shape[1])
    rows = [values.reshape(1, -1) for values in (norm_gain, decay_bias, head_gain, moe_gain)]
    operands = (
        tokens,
        rows[0],
        w_query,
        w_key,
        w_value,
        w_outgate,
        decay_in.T,
        decay_out,
        rows[1],
        gla_state,
        rows[2],
        w_output,
        rows[3],
        expert_ids.T,
        route_weight.T,
        expert_gate,
        expert_up,
        expert_down,
        shared_gate,
        shared_up,
        shared_down,
    )

    def held(values):
        return pltpu.VMEM(values.shape, values.dtype)

    scratch = [
        held(tokens),
        held(rows[0]),
        pltpu.VMEM((block, span), jnp.bfloat16),
        held(operands[6]),
        held(decay_out),
        held(rows[1]),
        held(rows[2]),
        held(w_output),
        held(rows[3]),
        held(operands[13]),
        held(operands[14]),
        pltpu.VMEM((width, 2 * (hidden_units + shared_units)), jnp.bfloat16),
        pltpu.VMEM((hidden_units + shared_units, width), jnp.bfloat16),
        pltpu.VMEM((2, width), jnp.float32),
        pltpu.VMEM((ep_size, 2, block), jnp.float32),
        pltpu.VMEM((ep_size, span // 128, 128), jnp.bfloat16),
        pltpu.VMEM((ep_size, span // 128, 128), jnp.bfloat16),
        pltpu.VMEM((DV // 128, 128), jnp.bfloat16),
        pltpu.VMEM((devices, DV // 128, 128), jnp.bfloat16),
        pltpu.VMEM((ep_size, block), jnp.bfloat16),
        pltpu.VMEM((ep_size, width), jnp.bfloat16),
        pltpu.VMEM((ep_size, width), jnp.bfloat16),
        pltpu.VMEM((devices, ep_size, block), jnp.bfloat16),
        pltpu.VMEM((ep_size, span // 128, 128), jnp.float32),
        pltpu.SemaphoreType.DMA((len(operands),)),
        pltpu.SemaphoreType.DMA((5,)),
        pltpu.SemaphoreType.DMA((5,)),
    ]
    result, new_state = pl.pallas_call(
        functools.partial(layer_kernel, ep_size, tp_size),
        out_shape=(
            pltpu.VMEM((ep_size, block), jnp.bfloat16),
            pltpu.VMEM(gla_state.shape, jnp.float32),
        ),
        in_specs=[pl.BlockSpec(memory_space=HBM)] * len(operands),
        out_specs=(pl.BlockSpec(memory_space=pltpu.VMEM),) * 2,
        scratch_shapes=scratch,
        compiler_params=pltpu.CompilerParams(
            collective_id=0, has_side_effects=True
        ),
    )(*operands)
    return pl.pallas_call(
        write_kernel,
        out_shape=(
            jax.ShapeDtypeStruct(result.shape, result.dtype),
            jax.ShapeDtypeStruct(new_state.shape, new_state.dtype),
        ),
        in_specs=[pl.BlockSpec(memory_space=pltpu.VMEM)] * 2,
        out_specs=(pl.BlockSpec(memory_space=HBM),) * 2,
        scratch_shapes=[pltpu.SemaphoreType.DMA((2,))],
        compiler_params=pltpu.CompilerParams(vmem_limit_bytes=8 * 1024 * 1024),
    )(result, new_state)


def chosen_device(*args):
    tokens, w_query, w_output, expert_gate = args[0], args[2], args[11], args[15]
    ep_size = lax.axis_size("ep")
    fits = (
        tokens.shape[0] == 1
        and expert_gate.shape[0] == 1
        and w_query.shape[1] == DK
        and w_output.shape[1] % 128 == 0
        and ep_size % (args[18].shape[1] // min(128, args[18].shape[1])) == 0
    )
    return fused_device(*args) if fits else per_device(*args)


def solution(mesh):
    return jax.shard_map(
        chosen_device,
        mesh=mesh,
        in_specs=(
            P("ep", None),
            P(),
            P("ep", "tp"),
            P("ep", "tp"),
            P("ep", "tp"),
            P("ep", "tp"),
            P(),
            P(None, "tp"),
            P("tp"),
            P("ep", "tp", None, None),
            P(),
            P(None, "ep"),
            P(),
            P(),
            P(),
            P("ep", None, "tp"),
            P("ep", None, "tp"),
            P("ep", "tp", None),
            P(None, "tp"),
            P(None, "tp"),
            P("tp", None),
        ),
        out_specs=(P(None, "ep"), P("ep", "tp", None, None)),
        check_vma=False,
    )
```
